32 devices in a mesh: sp: 8 (over z, core), tp: 4 (over y, x).
Axes of the slice: x: 2, y: 2, z: 4, core: 2. Of those that a mesh axis runs over, the one named last changes fastest.
Arguments:
- queries: bfloat16 [2048, 1024], P('sp', 'tp'), may hold values from -250 to 250
- keys_values: bfloat16 [2, 2048, 256], P(None, 'sp'), may hold values from -8 to 8
- sink_logits: float32 [16], P('tp'), may hold values from 1 to 5
- proj_weight: bfloat16 [1024, 2048], P('tp'), may hold values from -0.75 to 0.75
- residual: bfloat16 [2048, 2048], P('sp', 'tp'), may hold values from -6 to 6
- norm_gain: float32 [2048], replicated, may hold values from 0.1 to 1.9
- routes: int32 [2048, 2], P('sp'), may hold values from 0 to 7, all different within a row; in each aligned block of 256 rows (0 to 255, 256 to 511, ...) at most 128 rows name the same one
- route_weights: float32 [2048, 2], P('sp'), may hold values from 0.2 to 1
- gate_weight: bfloat16 [8, 2048, 2048], P('sp', None, 'tp'), may hold values from -0.125 to 0.125
- up_weight: bfloat16 [8, 2048, 2048], P('sp', None, 'tp'), may hold values from -0.125 to 0.125
- down_weight: bfloat16 [8, 2048, 2048], P('sp', None, 'tp'), may hold values from -0.125 to 0.125
- shared_gate: bfloat16 [2048, 2048], P(None, 'tp'), may hold values from -0.125 to 0.125
- shared_up: bfloat16 [2048, 2048], P(None, 'tp'), may hold values from -0.125 to 0.125
- shared_down: bfloat16 [2048, 2048], P(None, 'tp'), may hold values from -0.125 to 0.125
Outputs:
- output: bfloat16 [2048, 2048], P('sp', 'tp')
The draws below stay inside these ranges and needn't reach their ends.
Inputs may be any that keep to these rules, and one draw needn't show every extreme that they name: `routes`: the 2 experts of a position differ. In each aligned block of 256 positions no expert is named by more than 128 positions, and in some block one expert is named by exactly 128.
All inputs are finite; a program needn't handle non-finite values.
Results may differ from the reference program's by a relative error of at most 0.0067.
Values may be sent and summed in bfloat16 or wider, within the bound.
A program may use at most 64 MiB of HBM per device.

```python
import math
import jax
import jax.numpy as jnp
import numpy as np
from jax import lax

D = 2048
HEADS = 16
KV_HEADS = 4
HEAD_WIDTH = 64
D_EXP = 2048
WINDOW = 128
TOP_K = 2
TOK_DEV = 256
TOKENS = 2048
EXPERTS = 8
CAP = 128
N_SP = 8


def attention_draws(key):
    query_seed = jax.random.fold_in(key, 101)
    value_seed = jax.random.fold_in(key, 202)
    keys_values = jax.random.normal(value_seed, (2, TOKENS, KV_HEADS * HEAD_WIDTH), jnp.float32)
    queries = jax.random.normal(query_seed, (TOKENS, HEADS * HEAD_WIDTH), jnp.float32)
    keys_values = jnp.clip(keys_values, -8.0, 8.0)
    return (queries, keys_values)


def draw_queries(key, part):
    return attention_draws(key)[0].astype(jnp.bfloat16)


def draw_keys_values(key, part):
    return attention_draws(key)[1].astype(jnp.bfloat16)


def block_scale(stream_key, dims, shards, smallest, largest):
    loudness = 1.0
    for dim, parts in shards:
        heights = jax.random.uniform(jax.random.fold_in(jax.random.fold_in(stream_key, 6), dim), (parts,), jnp.float32, smallest / len(shards), largest / len(shards))
        loudness = loudness * jnp.repeat(jnp.exp(heights), dims[dim] // parts).reshape((-1,) + (1,) * (len(dims) - 1 - dim))
    return loudness


def deal_out(key, own, number, rows, count, top, most, skew):
    sequence = jax.random.permutation(key, count)
    packed, common = shares(count, rows * top, most, skew, True), shares(count, rows * top, most, skew, False)
    places = jnp.arange(count)

    def named(tallies, offset_by):
        used = int((tallies > 0).sum())
        fixed = max(1, used // 4)
        shifted = fixed + (places - fixed + offset_by * (used - fixed)) % max(1, count - fixed)
        return jnp.zeros((count,), jnp.int32).at[sequence[jnp.where(places < fixed, places, shifted)]].set(jnp.asarray(tallies, jnp.int32))

    tallies = jnp.where(number % 4 == 0, named(packed, number // 4), named(common, number - number // 4 - 1))
    mixed = jax.random.permutation(jax.random.fold_in(own, 3), count)
    donor, receiver = mixed[0:count // 2 * 2:2], mixed[1:count // 2 * 2:2]
    slack = jnp.minimum(tallies[donor] - 1, most - tallies[receiver]) // 2
    slack = jnp.where((donor == sequence[0]) | (receiver == sequence[0]) | (tallies[receiver] == 0), 0, jnp.maximum(slack, 0))
    shifted = jax.random.randint(jax.random.fold_in(own, 4), (count // 2,), 0, 1 << 20) % (slack + 1)
    tallies = tallies.at[donor].add(-shifted).at[receiver].add(shifted)
    labels = jnp.searchsorted(jnp.cumsum(tallies), jnp.arange(rows * top), side="right").astype(jnp.int32)
    grid = labels.reshape(top, rows).T
    grid = grid[jax.random.permutation(jax.random.fold_in(own, 1), rows)]
    offset_by = jax.random.randint(jax.random.fold_in(own, 2), (rows, 1), 0, top)
    return jnp.take_along_axis(grid, (jnp.arange(top)[None, :] + offset_by) % top, axis=1)


def shares(number_of, total, limit, skew, full):
    portions = [(1 << 20) // math.isqrt(standing ** skew) + 1 for standing in range(1, number_of + 1)]
    largest = limit if full else min(limit, max(-(-total // number_of), total * portions[0] // sum(portions)))
    least = 1 if total - largest >= number_of - 1 else 0
    given, surplus = [largest] + [least] * (number_of - 1), total - largest - least * (number_of - 1)
    while surplus > 0:
        free = [i for i in range(1, number_of) if given[i] < largest] or [i for i in range(1, number_of) if given[i] < limit]
        mass, remaining = sum([portions[i] for i in free]), surplus
        for i in free:
            extra = min(limit - given[i], max(1, remaining * portions[i] // mass), surplus)
            given[i] = given[i] + extra
            surplus = surplus - extra
    return np.array(given)


def noise(own_key, dims, width, reach, shards=(), held_as=jnp.bfloat16):
    array = width * jax.random.normal(own_key, dims, jnp.float32)
    if shards:
        array = array * block_scale(own_key, dims, shards, -0.22, 0.18)
    return jnp.clip(array, -reach, reach).astype(held_as)


def setup_inputs(seed: int = 0) -> dict:
    key_of = jax.random.split(jax.random.key(seed), 15)
    queries = draw_queries(jax.random.fold_in(key_of[14], 71), 0)
    keys_values = draw_keys_values(jax.random.fold_in(key_of[14], 71), 0)
    sink_logits = jnp.clip(1.0 + 4.0 * jax.random.uniform(key_of[2], (HEADS,), jnp.float32) ** block_scale(key_of[2], (HEADS,), ((0, 4),), -0.2, 0.2), 1.0, 5.0)
    proj_weight = noise(key_of[3], (HEADS * HEAD_WIDTH, D), (HEADS * HEAD_WIDTH // 16) ** -0.5, 0.75, ((0, 4),))
    residual = noise(key_of[4], (TOKENS, D), 1.0, 6.0, ((0, 8), (1, 4)))
    norm_gain = jnp.clip(1.0 + 0.18 * jax.random.normal(key_of[5], (D,), jnp.float32), 0.1, 1.9)
    routes_keys = jax.random.split(jax.random.fold_in(key_of[6], 1), TOKENS // TOK_DEV)
    routes_turns = jax.random.permutation(jax.random.fold_in(key_of[6], 3), TOKENS // TOK_DEV)
    routes = jax.vmap(lambda own, number: deal_out(jax.random.fold_in(key_of[6], 2), own, number, TOK_DEV, EXPERTS, TOP_K, CAP, 1))(routes_keys, routes_turns).reshape((TOKENS, TOP_K))
    route_weights = jnp.clip(0.2 + 0.8 * jax.random.uniform(key_of[7], (TOKENS, TOP_K), jnp.float32) ** block_scale(key_of[7], (TOKENS, TOP_K), ((0, 8),), -0.2, 0.2), 0.2, 1.0)
    gate_weight = noise(key_of[8], (EXPERTS, D, D_EXP), D ** -0.5, 0.125, ((0, 8), (2, 4)))
    up_weight = noise(key_of[9], (EXPERTS, D, D_EXP), D ** -0.5, 0.125, ((0, 8), (2, 4)))
    down_weight = noise(key_of[10], (EXPERTS, D_EXP, D), D_EXP ** -0.5, 0.125, ((0, 8), (2, 4)))
    shared_gate = noise(key_of[11], (D, D_EXP), D ** -0.5, 0.125, ((1, 4),))
    shared_up = noise(key_of[12], (D, D_EXP), D ** -0.5, 0.125, ((1, 4),))
    shared_down = noise(key_of[13], (D_EXP, D), D_EXP ** -0.5, 0.125, ((1, 4),))
    return dict(queries=queries, keys_values=keys_values, sink_logits=sink_logits, proj_weight=proj_weight, residual=residual, norm_gain=norm_gain, routes=routes, route_weights=route_weights, gate_weight=gate_weight, up_weight=up_weight, down_weight=down_weight, shared_gate=shared_gate, shared_up=shared_up, shared_down=shared_down)


norm_eps = 1e-06

def attention_layer(queries, keys_values, sink_logits):
    blocks = TOKENS // WINDOW
    kv_group = HEADS // KV_HEADS
    query_blocks = queries.reshape(blocks, WINDOW, HEADS, HEAD_WIDTH)
    padded = jnp.concatenate([jnp.zeros((2, WINDOW, KV_HEADS * HEAD_WIDTH), keys_values.dtype), keys_values], axis=1)
    padded = padded.reshape(2, TOKENS + WINDOW, KV_HEADS, HEAD_WIDTH)
    earlier = padded[:, :TOKENS].reshape(2, blocks, WINDOW, KV_HEADS, HEAD_WIDTH)
    later = padded[:, WINDOW:].reshape(2, blocks, WINDOW, KV_HEADS, HEAD_WIDTH)
    banded = jnp.concatenate([earlier, later], axis=2)
    query_pos = jnp.arange(WINDOW, dtype=jnp.int32)[:, None]
    key_pos = jnp.arange(2 * WINDOW, dtype=jnp.int32)[None, :]
    distance = WINDOW + query_pos - key_pos
    absolute = jnp.arange(blocks, dtype=jnp.int32)[:, None, None] * WINDOW - WINDOW + key_pos[None]
    allowed = (distance >= 0)[None] & (distance < WINDOW)[None] & (absolute >= 0)

    def one_head(head_number):
        head_queries = lax.dynamic_index_in_dim(query_blocks, head_number, 2, keepdims=False)
        kv_number = head_number // kv_group
        head_keys = lax.dynamic_index_in_dim(banded[0], kv_number, 2, keepdims=False)
        head_values = lax.dynamic_index_in_dim(banded[1], kv_number, 2, keepdims=False)
        score_matrix = jnp.einsum('pvg,pug->pvu', head_queries.astype(jnp.float32), head_keys.astype(jnp.float32)) * HEAD_WIDTH ** (-0.5)
        masked = jnp.where(allowed, score_matrix, -jnp.inf)
        sink_value = sink_logits[head_number].astype(jnp.float32)
        highest = jnp.maximum(lax.optimization_barrier(jnp.max(masked, axis=-1, keepdims=True)), sink_value)
        weights_exp = jnp.exp(masked - highest)
        denominator = lax.optimization_barrier(jnp.sum(weights_exp, axis=-1, keepdims=True)) + jnp.exp(sink_value - highest)
        softmax_weights = (weights_exp / denominator).astype(jnp.bfloat16)
        attended_values = jnp.einsum('ugj,ujs->ugs', softmax_weights.astype(jnp.float32), head_values.astype(jnp.float32))
        return attended_values.astype(jnp.bfloat16)
    per_head = lax.map(one_head, jnp.arange(HEADS, dtype=jnp.int32))
    return jnp.transpose(per_head, (1, 2, 0, 3)).reshape(TOKENS, HEADS * HEAD_WIDTH)

def reference(queries, keys_values, sink_logits, proj_weight, residual, norm_gain, routes, route_weights, gate_weight, up_weight, down_weight, shared_gate, shared_up, shared_down):
    attended_values = attention_layer(queries, keys_values, sink_logits)
    stream_f = jnp.dot(attended_values, proj_weight, preferred_element_type=jnp.float32) + residual.astype(jnp.float32)
    stream = stream_f.astype(jnp.bfloat16)
    stream_wide = stream.astype(jnp.float32)
    row_scale = lax.rsqrt(lax.optimization_barrier(jnp.mean(stream_wide * stream_wide, axis=-1)) + norm_eps)
    gain_col = norm_gain.astype(jnp.float32)[:, None]
    slots = N_SP * CAP
    flat_routes = routes.reshape(-1).astype(jnp.int32)
    assigned = flat_routes.shape[0]
    onehot = (flat_routes[:, None] == jnp.arange(EXPERTS, dtype=jnp.int32)[None, :]).astype(jnp.int32)
    before = jnp.cumsum(onehot, axis=0) - onehot
    slot_rank = lax.optimization_barrier(jnp.sum(before * onehot, axis=1)).astype(jnp.int32)
    token_of = (jnp.arange(assigned, dtype=jnp.int32) // TOP_K).astype(jnp.int32)
    slot_owner = jnp.full((EXPERTS, slots), TOKENS, jnp.int32).at[flat_routes, slot_rank].set(token_of)

    def one_expert(expert):
        owners = slot_owner[expert]
        rows = jnp.take(stream, owners, axis=0, mode='fill', fill_value=0)
        scales = jnp.take(row_scale, owners, axis=0, mode='fill', fill_value=0)
        gate_eff = (gain_col * gate_weight[expert].astype(jnp.float32)).astype(jnp.bfloat16)
        up_eff = (gain_col * up_weight[expert].astype(jnp.float32)).astype(jnp.bfloat16)
        gate_val = scales[:, None] * jnp.dot(rows, gate_eff, preferred_element_type=jnp.float32)
        up_val = scales[:, None] * jnp.dot(rows, up_eff, preferred_element_type=jnp.float32)
        hidden = (jax.nn.silu(gate_val) * up_val).astype(jnp.bfloat16)
        return jnp.dot(hidden, down_weight[expert], preferred_element_type=jnp.float32).astype(jnp.bfloat16)
    expert_out = lax.map(one_expert, jnp.arange(EXPERTS, dtype=jnp.int32))
    picked = expert_out[flat_routes, slot_rank].reshape(TOKENS, TOP_K, D)
    routed = lax.optimization_barrier(jnp.sum(route_weights.astype(jnp.float32)[:, :, None] * picked.astype(jnp.float32), axis=1))
    shared_gate_eff = (gain_col * shared_gate.astype(jnp.float32)).astype(jnp.bfloat16)
    shared_up_eff = (gain_col * shared_up.astype(jnp.float32)).astype(jnp.bfloat16)
    shared_gate_val = row_scale[:, None] * jnp.dot(stream, shared_gate_eff, preferred_element_type=jnp.float32)
    shared_up_val = row_scale[:, None] * jnp.dot(stream, shared_up_eff, preferred_element_type=jnp.float32)
    shared_hidden = (jax.nn.silu(shared_gate_val) * shared_up_val).astype(jnp.bfloat16)
    shared_out = jnp.dot(shared_hidden, shared_down, preferred_element_type=jnp.float32)
    return (stream_wide + shared_out + routed).astype(jnp.bfloat16)
```

```python
import functools

import jax
import jax.numpy as jnp
from jax import lax
from jax.experimental import pallas as pl
from jax.experimental.pallas import tpu as pltpu
from jax.sharding import PartitionSpec as P

D = 2048
HEADS = 16
KV_HEADS = 4
HEAD_WIDTH = 64
WINDOW = 128
TOP_K = 2
EXP_DEV = 1
TOK_DEV = 256


norm_eps = 1e-06


def passed_along(value, axis, steps):
    count = lax.axis_size(axis)
    initial, last = (max(0, -steps), min(count, count - steps))
    return lax.ppermute(value, axis, [(source, source + steps) for source in range(initial, last)])


MESH = pl.DeviceIdType.MESH
CORES = 2
LAG = 3


def expert_kernel(
    sp_count,
    tp_count,
    cap,
    stream_ref,
    routes_ref,
    routes_row_ref,
    weights_ref,
    gain_ref,
    gate_ref,
    up_ref,
    down_ref,
    sgate_ref,
    sup_ref,
    sdown_ref,
    out_ref,
    wgu,
    wd,
    sgu,
    sd,
    full,
    picks,
    picked_full,
    arrived,
    hid,
    shid,
    eout,
    returned,
    pos,
    acc,
    load_sem,
    stream_sems,
    z_send,
    z_recv,
    fwd_send,
    fwd_recv,
    hid_send,
    hid_recv,
    sh_sems,
    ret_send,
    ret_recv,
):
    s = lax.axis_index("sp")
    t = lax.axis_index("tp")
    rows, width = stream_ref.shape
    depth = width * tp_count
    chips = sp_count // CORES
    z, core = s // CORES, lax.rem(s, CORES)
    cols = pl.ds(pl.multiple_of(t * width, width), width)
    wide = pl.ds(0, (tp_count - 1) * width)

    def source(i):
        return lax.rem(z + i // CORES, chips) * CORES + lax.rem(core + lax.rem(i, CORES), CORES)

    def target(i):
        return (
            lax.rem(z - i // CORES + chips, chips) * CORES
            + lax.rem(core - lax.rem(i, CORES) + CORES, CORES)
        )

    def tp_copies(ref, send_sem, recv_sem):
        for j in range(1, tp_count):
            pltpu.make_async_remote_copy(
                src_ref=ref,
                dst_ref=ref,
                send_sem=send_sem,
                recv_sem=recv_sem,
                device_id={"tp": lax.rem(t + j, tp_count)},
                device_id_type=MESH,
            ).start()

    def tp_wait(ref, send_sem, recv_sem):
        return pltpu.make_async_remote_copy(
            src_ref=ref,
            dst_ref=ref,
            send_sem=send_sem,
            recv_sem=recv_sem,
            device_id={"tp": lax.rem(t + 1, tp_count)},
            device_id_type=MESH,
        )

    def sp_copy(src, dst, send_sem, recv_sem, device):
        return pltpu.make_async_remote_copy(
            src_ref=src,
            dst_ref=dst,
            send_sem=send_sem,
            recv_sem=recv_sem,
            device_id={"sp": device},
            device_id_type=MESH,
        )

    left, right = pl.ds(0, width), pl.ds(width, width)
    loads = [
        pltpu.make_async_copy(src, dst, load_sem.at[n])
        for n, (src, dst) in enumerate(
            (
                (gate_ref.at[0], wgu.at[:, left]),
                (up_ref.at[0], wgu.at[:, right]),
                (sgate_ref, sgu.at[:, left]),
                (sup_ref, sgu.at[:, right]),
                (down_ref.at[0], wd),
                (sdown_ref, sd),
            )
        )
    ]
    for load in loads:
        load.start()

    barrier = pltpu.get_barrier_semaphore()
    for j in range(1, tp_count):
        pl.semaphore_signal(
            barrier, inc=1, device_id={"tp": lax.rem(t + j, tp_count)}, device_id_type=MESH
        )

    @pl.loop(1, sp_count)
    def _(i):
        pl.semaphore_signal(
            barrier, inc=1, device_id={"sp": lax.rem(s + i, sp_count)}, device_id_type=MESH
        )

    full[:, cols] = stream_ref[...]

    named = lax.broadcasted_iota(jnp.int32, (sp_count, rows), 0)
    member = named == routes_row_ref[0:1, :]
    for k in range(1, routes_row_ref.shape[0]):
        member = member | (named == routes_row_ref[k : k + 1, :])
    earlier = lax.broadcasted_iota(jnp.int32, (rows, rows), 0) < lax.broadcasted_iota(
        jnp.int32, (rows, rows), 1
    )
    rank = jnp.dot(
        jnp.where(member, 1.0, 0.0).astype(jnp.bfloat16),
        jnp.where(earlier, 1.0, 0.0).astype(jnp.bfloat16),
        preferred_element_type=jnp.float32,
    )
    pos[...] = jnp.where(member, rank.astype(jnp.int32), -1)

    def chooser(e):
        hit = lax.broadcasted_iota(jnp.int32, (cap, rows), 0) == pos[pl.ds(e, 1), :]
        return jnp.where(hit, 1.0, 0.0).astype(jnp.bfloat16)

    pl.semaphore_wait(barrier, sp_count + tp_count - 2)

    tp_copies(full.at[:, cols], stream_sems.at[0], stream_sems.at[1])

    @pl.loop(CORES, sp_count)
    def _(i):
        e = target(i)
        picks[e] = jnp.dot(
            chooser(e), stream_ref[...], preferred_element_type=jnp.float32
        ).astype(jnp.bfloat16)
        sp_copy(picks.at[e], arrived.at[s, :, cols], z_send.at[e], z_recv.at[s], e).start()

    def scale_weights(w):
        step = 128

        @pl.loop(0, depth // step)
        def _(r):
            part = pl.ds(pl.multiple_of(r * step, step), step)
            w[part, :] = (gain_ref[part, :] * w[part, :].astype(jnp.float32)).astype(jnp.bfloat16)

    loads[0].wait()
    loads[1].wait()
    scale_weights(wgu)

    stream_wait = tp_wait(full.at[:, wide], stream_sems.at[0], stream_sems.at[1])
    stream_wait.wait_recv()
    sibling = target(1)
    picked_full[...] = jnp.dot(
        chooser(sibling), full[...], preferred_element_type=jnp.float32
    ).astype(jnp.bfloat16)
    sp_copy(picked_full, arrived.at[s], z_send.at[sibling], z_recv.at[s], sibling).start()
    arrived[s] = jnp.dot(chooser(s), full[...], preferred_element_type=jnp.float32).astype(
        jnp.bfloat16
    )

    def gated(x, w):
        wide_x = x.astype(jnp.float32)
        scale = lax.rsqrt(jnp.sum(wide_x * wide_x, axis=-1, keepdims=True) / depth + norm_eps)
        sums = jnp.dot(x, w[...], preferred_element_type=jnp.float32)
        gate = scale * sums[:, :width]
        return (gate / (1.0 + jnp.exp(-gate)) * (scale * sums[:, width:])).astype(jnp.bfloat16)

    def hidden_of(src):
        hid[src, :, cols] = gated(arrived[src], wgu)
        tp_copies(hid.at[src, :, cols], hid_send.at[src], hid_recv.at[src])

    hidden_of(s)
    loads[2].wait()
    loads[3].wait()
    scale_weights(sgu)
    half = rows // 2

    @pl.loop(0, 2)
    def _(h):
        part = pl.ds(pl.multiple_of(h * half, half), half)
        shid[part, cols] = gated(full[part, :], sgu)

    tp_copies(shid.at[:, cols], sh_sems.at[0], sh_sems.at[1])

    @pl.loop(CORES, sp_count)
    def _(i):
        src = source(i)
        mine = arrived.at[src, :, cols]
        sp_copy(mine, mine, z_send.at[src], z_recv.at[src], src).wait_recv()
        tp_copies(mine, fwd_send.at[src], fwd_recv.at[src])

    loads[4].wait()
    loads[5].wait()

    @pl.loop(1, sp_count + LAG)
    def _(i):
        @pl.when(i < sp_count)
        def _():
            src = source(i)

            @pl.when(i < CORES)
            def _():
                mine = arrived.at[src]
                sp_copy(mine, mine, z_send.at[src], z_recv.at[src], src).wait_recv()

            @pl.when(i >= CORES)
            def _():
                tp_wait(
                    arrived.at[src, :, wide], fwd_send.at[src], fwd_recv.at[src]
                ).wait_recv()

            hidden_of(src)

        @pl.when(i >= LAG)
        def _():
            src = source(i - LAG)
            tp_wait(hid.at[src, :, wide], hid_send.at[src], hid_recv.at[src]).wait_recv()
            result = jnp.dot(hid[src], wd[...], preferred_element_type=jnp.float32).astype(
                jnp.bfloat16
            )

            @pl.when(i == LAG)
            def _():
                returned[s] = result

            @pl.when(i > LAG)
            def _():
                eout[src] = result
                sp_copy(
                    eout.at[src], returned.at[s], ret_send.at[src], ret_recv.at[s], src
                ).start()

    tp_wait(shid.at[:, wide], sh_sems.at[0], sh_sems.at[1]).wait_recv()
    acc[...] = stream_ref[...].astype(jnp.float32) + jnp.dot(
        shid[...], sd[...], preferred_element_type=jnp.float32
    )

    @pl.loop(0, sp_count)
    def _(i):
        e = target(i)

        @pl.when(i > 0)
        def _():
            mine = returned.at[e]
            sp_copy(mine, mine, ret_send.at[e], ret_recv.at[e], e).wait_recv()

        picked = lax.dot_general(
            chooser(e), returned[e], (((0,), (0,)), ((), ())), preferred_element_type=jnp.float32
        )
        weight = jnp.sum(
            jnp.where(routes_ref[...] == e, weights_ref[...], 0.0), axis=1, keepdims=True
        )
        acc[...] += weight * picked

    out_ref[...] = acc[...].astype(out_ref.dtype)

    stream_wait.wait_send()
    tp_wait(shid.at[:, wide], sh_sems.at[0], sh_sems.at[1]).wait_send()

    @pl.loop(0, sp_count)
    def _(i):
        e = target(i)
        tp_wait(hid.at[e, :, wide], hid_send.at[e], hid_recv.at[e]).wait_send()

        @pl.when(i == 1)
        def _():
            sp_copy(picked_full, picked_full, z_send.at[e], z_recv.at[e], e).wait_send()

        @pl.when(i >= CORES)
        def _():
            sp_copy(picks.at[e], picks.at[e], z_send.at[e], z_recv.at[e], e).wait_send()
            tp_wait(arrived.at[e, :, wide], fwd_send.at[e], fwd_recv.at[e]).wait_send()

        @pl.when(i > 0)
        def _():
            sp_copy(eout.at[e], eout.at[e], ret_send.at[e], ret_recv.at[e], e).wait_send()


def expert_layer(stream, routes, route_weights, norm_gain, gate, up, down, sgate, sup, sdown):
    sp_count = lax.axis_size("sp")
    tp_count = lax.axis_size("tp")
    rows, width = stream.shape
    depth = width * tp_count
    cap = 2 * rows * TOP_K // sp_count
    bf16 = jnp.bfloat16
    vmem = pl.BlockSpec(memory_space=pltpu.VMEM)
    hbm = pl.BlockSpec(memory_space=pl.ANY)
    dma = pltpu.SemaphoreType.DMA
    return pl.pallas_call(
        functools.partial(expert_kernel, sp_count, tp_count, cap),
        out_shape=jax.ShapeDtypeStruct((rows, width), bf16),
        in_specs=[vmem] * 5 + [hbm] * 6,
        out_specs=vmem,
        scratch_shapes=[
            pltpu.VMEM((depth, 2 * width), bf16),
            pltpu.VMEM((depth, width), bf16),
            pltpu.VMEM((depth, 2 * width), bf16),
            pltpu.VMEM((depth, width), bf16),
            pltpu.VMEM((rows, depth), bf16),
            pltpu.VMEM((sp_count, cap, width), bf16),
            pltpu.VMEM((cap, depth), bf16),
            pltpu.VMEM((sp_count, cap, depth), bf16),
            pltpu.VMEM((sp_count, cap, depth), bf16),
            pltpu.VMEM((rows, depth), bf16),
            pltpu.VMEM((sp_count, cap, width), bf16),
            pltpu.VMEM((sp_count, cap, width), bf16),
            pltpu.VMEM((sp_count, rows), jnp.int32),
            pltpu.VMEM((rows, width), jnp.float32),
            dma((6,)),
            dma((2,)),
            dma((sp_count,)),
            dma((sp_count,)),
            dma((sp_count,)),
            dma((sp_count,)),
            dma((sp_count,)),
            dma((sp_count,)),
            dma((2,)),
            dma((sp_count,)),
            dma((sp_count,)),
        ],
        compiler_params=pltpu.CompilerParams(
            collective_id=0, has_side_effects=True, vmem_limit_bytes=56 * 1024 * 1024
        ),
    )(
        stream,
        routes,
        routes.T,
        route_weights,
        norm_gain[:, None],
        gate,
        up,
        down,
        sgate,
        sup,
        sdown,
    )


def per_device(
    queries,
    keys_values,
    sink_logits,
    proj_weight,
    residual,
    norm_gain,
    routes,
    route_weights,
    gate_weight,
    up_weight,
    down_weight,
    shared_gate,
    shared_up,
    shared_down,
):
    tp_index = lax.axis_index("tp")
    sp_index = lax.axis_index("sp")
    sp_count = lax.axis_size("sp")
    tp_count = lax.axis_size("tp")
    heads_here = sink_logits.shape[0]
    col_width = residual.shape[1]
    blocks = TOK_DEV // WINDOW
    kv_group = HEADS // KV_HEADS
    earlier_keys = passed_along(keys_values[:, TOK_DEV - WINDOW :, :], "sp", 1)
    extended = jnp.concatenate([earlier_keys, keys_values], axis=1)
    extended = extended.reshape(2, TOK_DEV + WINDOW, KV_HEADS, HEAD_WIDTH)
    head_ids = tp_index * heads_here + jnp.arange(heads_here, dtype=jnp.int32)
    chosen = jnp.take(extended, head_ids // kv_group, axis=2)
    earlier = chosen[:, :TOK_DEV].reshape(2, blocks, WINDOW, heads_here, HEAD_WIDTH)
    later = chosen[:, WINDOW:].reshape(2, blocks, WINDOW, heads_here, HEAD_WIDTH)
    banded = jnp.concatenate([earlier, later], axis=2)
    query_blocks = queries.reshape(blocks, WINDOW, heads_here, HEAD_WIDTH)
    score_matrix = jnp.einsum(
        "bqhd,bkhd->bhqk", query_blocks, banded[0], preferred_element_type=jnp.float32
    ) * HEAD_WIDTH ** (-0.5)
    query_pos = jnp.arange(WINDOW, dtype=jnp.int32)[:, None]
    key_pos = jnp.arange(2 * WINDOW, dtype=jnp.int32)[None, :]
    distance = WINDOW + query_pos - key_pos
    absolute = (
        sp_index * TOK_DEV
        + jnp.arange(blocks, dtype=jnp.int32)[:, None, None] * WINDOW
        - WINDOW
        + key_pos[None]
    )
    allowed = (distance >= 0)[None] & (distance < WINDOW)[None] & (absolute >= 0)
    masked = jnp.where(allowed[:, None], score_matrix, -jnp.inf)
    sink_value = sink_logits[None, :, None, None]
    highest = jnp.maximum(jnp.max(masked, axis=-1, keepdims=True), sink_value)
    weights_exp = jnp.exp(masked - highest)
    denominator = jnp.sum(weights_exp, axis=-1, keepdims=True) + jnp.exp(sink_value - highest)
    softmax_weights = (weights_exp / denominator).astype(jnp.bfloat16)
    attended_values = jnp.einsum(
        "bhqk,bkhd->bqhd", softmax_weights, banded[1], preferred_element_type=jnp.float32
    )
    attended_values = attended_values.astype(jnp.bfloat16).reshape(TOK_DEV, heads_here * HEAD_WIDTH)
    attended_all = lax.all_gather(attended_values, "tp", axis=1, tiled=True)
    weight_rows = proj_weight.shape[0]
    column_share = lax.all_to_all(
        proj_weight.reshape(weight_rows, tp_count, col_width),
        "tp",
        split_axis=1,
        concat_axis=0,
        tiled=True,
    )
    column_share = column_share.reshape(HEADS * HEAD_WIDTH, col_width)
    feature_sum = jnp.dot(attended_all, column_share, preferred_element_type=jnp.float32)
    stream_cols = (feature_sum + residual.astype(jnp.float32)).astype(jnp.bfloat16)
    return expert_layer(
        stream_cols,
        routes,
        route_weights,
        norm_gain,
        gate_weight,
        up_weight,
        down_weight,
        shared_gate,
        shared_up,
        shared_down,
    )


def solution(mesh):
    placed = (
        P("sp", "tp"),
        P(None, "sp", None),
        P("tp"),
        P("tp", None),
        P("sp", "tp"),
        P(),
        P("sp", None),
        P("sp", None),
        P("sp", None, "tp"),
        P("sp", None, "tp"),
        P("sp", None, "tp"),
        P(None, "tp"),
        P(None, "tp"),
        P(None, "tp"),
    )
    return jax.shard_map(
        per_device, mesh=mesh, in_specs=placed, out_specs=P("sp", "tp"), check_vma=False
    )
```

```python
import functools

import jax
import jax.numpy as jnp
from jax import lax
from jax.experimental import pallas as pl
from jax.experimental.pallas import tpu as pltpu
from jax.sharding import PartitionSpec as P

D = 2048
HEADS = 16
KV_HEADS = 4
HEAD_WIDTH = 64
WINDOW = 128
TOP_K = 2


norm_eps = 1e-06


MESH = pl.DeviceIdType.MESH
CORES = 2
NEAR = 4
LAG = 3


def expert_kernel(
    sp_count,
    tp_count,
    cap,
    queries_ref,
    kv_ref,
    sink_ref,
    residual_ref,
    routes_row_ref,
    weights_row_ref,
    gain_ref,
    proj_ref,
    gate_ref,
    up_ref,
    down_ref,
    sgate_ref,
    sup_ref,
    sdown_ref,
    out_ref,
    wgu,
    wd,
    sgu,
    sd,
    full,
    picks,
    picked_full,
    arrived,
    hid,
    shid,
    eout,
    returned,
    pos,
    acc,
    stream_ref,
    halo,
    banded,
    attended,
    columns,
    load_sem,
    front_send,
    front_recv,
    stream_send,
    stream_recv,
    z_send,
    z_recv,
    fwd_send,
    fwd_recv,
    hid_send,
    hid_recv,
    sh_send,
    sh_recv,
    ret_send,
    ret_recv,
):
    s = lax.axis_index("sp")
    t = lax.axis_index("tp")
    rows, width = residual_ref.shape
    depth = width * tp_count
    chips = sp_count // CORES
    z, core = s // CORES, lax.rem(s, CORES)
    cols = pl.ds(pl.multiple_of(t * width, width), width)
    wide = pl.ds(0, (tp_count - 1) * width)

    def offset(i):
        step = i // CORES
        return (step + 1) // 2 * (2 * lax.rem(step, 2) - 1)

    def source(i):
        return lax.rem(z + offset(i) + chips, chips) * CORES + lax.rem(
            core + lax.rem(i, CORES), CORES
        )

    def target(i):
        return lax.rem(z - offset(i) + chips, chips) * CORES + lax.rem(
            core - lax.rem(i, CORES) + CORES, CORES
        )

    square = tp_count == 4
    near = min(NEAR, sp_count)
    beside = 2 * (t // 2) + 1 - lax.rem(t, 2)
    across = lax.rem(t + 2, tp_count)

    def shard(n):
        return pl.ds(pl.multiple_of(n * width, width), width)

    def tp_copy(ref, send_sem, recv_sem, device):
        return pltpu.make_async_remote_copy(
            src_ref=ref,
            dst_ref=ref,
            send_sem=send_sem,
            recv_sem=recv_sem,
            device_id={"tp": device},
            device_id_type=MESH,
        )

    def tp_start(ref, send_sem, recv):
        mine = ref.at[:, cols]
        if square:
            tp_copy(mine, send_sem, recv.at[0], beside).start()
            tp_copy(mine, send_sem, recv.at[1], across).start()
        else:
            for j in range(1, tp_count):
                tp_copy(mine, send_sem, recv.at[2], lax.rem(t + j, tp_count)).start()

    def tp_relay(ref, send_sem, recv):
        if square:
            half = ref.shape[0] // 2
            tp_copy(ref.at[:, shard(beside)], send_sem, recv.at[0], beside).wait_recv()
            first = ref.at[pl.ds(0, half), shard(beside)]
            tp_copy(first, send_sem, recv.at[2], across).start()
            tp_copy(ref.at[:, shard(across)], send_sem, recv.at[1], across).wait_recv()
            second = ref.at[pl.ds(half, half), shard(across)]
            tp_copy(second, send_sem, recv.at[2], beside).start()

    def tp_finish(ref, send_sem, recv):
        part = ref.at[:, cols] if square else ref.at[:, wide]
        tp_copy(part, send_sem, recv.at[2], across).wait_recv()

    def tp_sent(ref, send_sem, recv):
        tp_copy(ref.at[:, wide], send_sem, recv.at[2], across).wait_send()

    def sp_copy(src, dst, send_sem, recv_sem, device):
        return pltpu.make_async_remote_copy(
            src_ref=src,
            dst_ref=dst,
            send_sem=send_sem,
            recv_sem=recv_sem,
            device_id={"sp": device},
            device_id_type=MESH,
        )

    lanes = proj_ref.shape[0]
    left, right = pl.ds(0, width), pl.ds(width, width)
    loads = [
        pltpu.make_async_copy(src, dst, load_sem.at[n])
        for n, (src, dst) in enumerate(
            (
                (gate_ref.at[0], wgu.at[:, left]),
                (up_ref.at[0], wgu.at[:, right]),
                (sgate_ref, sgu.at[:, left]),
                (sup_ref, sgu.at[:, right]),
                (down_ref.at[0], wd),
                (sdown_ref, sd),
                (proj_ref.at[:, cols], columns.at[pl.ds(t * lanes, lanes), :]),
            )
        )
    ]
    for load in loads[-1:] + loads[:-1]:
        load.start()

    barrier = pltpu.get_barrier_semaphore()
    for j in range(1, tp_count):
        pl.semaphore_signal(
            barrier, inc=1, device_id={"tp": lax.rem(t + j, tp_count)}, device_id_type=MESH
        )

    @pl.loop(1, sp_count)
    def _(i):
        pl.semaphore_signal(
            barrier, inc=1, device_id={"sp": lax.rem(s + i, sp_count)}, device_id_type=MESH
        )

    named = lax.broadcasted_iota(jnp.int32, (sp_count, rows), 0)
    member = named == routes_row_ref[0:1, :]
    for k in range(1, routes_row_ref.shape[0]):
        member = member | (named == routes_row_ref[k : k + 1, :])
    earlier = lax.broadcasted_iota(jnp.int32, (rows, rows), 0) < lax.broadcasted_iota(
        jnp.int32, (rows, rows), 1
    )
    rank = jnp.dot(
        jnp.where(member, 1.0, 0.0).astype(jnp.bfloat16),
        jnp.where(earlier, 1.0, 0.0).astype(jnp.bfloat16),
        preferred_element_type=jnp.float32,
    )
    pos[...] = jnp.where(member, rank.astype(jnp.int32), -1)

    def chooser(e):
        hit = lax.broadcasted_iota(jnp.int32, (cap, rows), 0) == pos[pl.ds(e, 1), :]
        return jnp.where(hit, 1.0, 0.0).astype(jnp.bfloat16)

    pl.semaphore_wait(barrier, sp_count + tp_count - 2)

    for j in range(1, tp_count):
        peer = lax.rem(t + j, tp_count)
        pltpu.make_async_remote_copy(
            src_ref=proj_ref.at[:, shard(peer)],
            dst_ref=columns.at[pl.ds(t * lanes, lanes), :],
            send_sem=front_send.at[1],
            recv_sem=front_recv.at[1],
            device_id={"tp": peer},
            device_id_type=MESH,
        ).start()

    kv_width = kv_ref.shape[2]
    blocks = rows // WINDOW
    following = lax.rem(s + 1, sp_count)
    tail_copy = sp_copy(
        kv_ref.at[:, pl.ds(rows - WINDOW, WINDOW), :],
        halo,
        front_send.at[0],
        front_recv.at[0],
        following,
    )

    @pl.when(s < sp_count - 1)
    def _():
        tail_copy.start()

    @pl.when(s == 0)
    def _():
        halo[...] = jnp.zeros_like(halo)

    @pl.when(s > 0)
    def _():
        tail_copy.wait_recv()

    heads_here = sink_ref.shape[1]
    kv_group = HEADS // KV_HEADS
    query_pos = lax.broadcasted_iota(jnp.int32, (WINDOW, 2 * WINDOW), 0)
    key_pos = lax.broadcasted_iota(jnp.int32, (WINDOW, 2 * WINDOW), 1)
    distance = WINDOW + query_pos - key_pos
    inside = (distance >= 0) & (distance < WINDOW)
    for head in range(heads_here):
        if head % kv_group == 0:
            kv_head = (t * heads_here + head) // kv_group
            for ref, first, count in ((halo, 0, WINDOW), (kv_ref, WINDOW, rows)):
                chosen = ref[:, :, :HEAD_WIDTH].astype(jnp.float32)
                for n in range(1, kv_width // HEAD_WIDTH):
                    other = ref[:, :, n * HEAD_WIDTH : (n + 1) * HEAD_WIDTH].astype(jnp.float32)
                    chosen = jnp.where(kv_head == n, other, chosen)
                banded[:, first : first + count, :] = chosen.astype(jnp.bfloat16)
        for block in range(blocks):
            here = slice(block * WINDOW, (block + 1) * WINDOW)
            near_keys = slice(block * WINDOW, (block + 2) * WINDOW)
            lane = slice(head * HEAD_WIDTH, (head + 1) * HEAD_WIDTH)
            scores = lax.dot_general(
                queries_ref[here, lane],
                banded[0, near_keys, :],
                (((1,), (1,)), ((), ())),
                preferred_element_type=jnp.float32,
            ) * HEAD_WIDTH ** (-0.5)
            allowed = inside & (key_pos + (s * rows + (block - 1) * WINDOW) >= 0)
            masked = jnp.where(allowed, scores, -jnp.inf)
            sink = sink_ref[0:1, head : head + 1]
            highest = jnp.maximum(jnp.max(masked, axis=-1, keepdims=True), sink)
            raised = jnp.exp(masked - highest)
            total = jnp.sum(raised, axis=-1, keepdims=True) + jnp.exp(sink - highest)
            attended[t, here, lane] = jnp.dot(
                (raised / total).astype(jnp.bfloat16),
                banded[1, near_keys, :],
                preferred_element_type=jnp.float32,
            ).astype(jnp.bfloat16)

    mine = attended.at[t]
    for j in range(1, tp_count):
        tp_copy(mine, front_send.at[2], front_recv.at[2], lax.rem(t + j, tp_count)).start()
    others = attended.at[pl.ds(0, tp_count - 1)]
    attended_wait = tp_copy(others, front_send.at[2], front_recv.at[2], across)
    most = columns.at[pl.ds(0, (tp_count - 1) * lanes), :]
    columns_wait = tp_copy(most, front_send.at[1], front_recv.at[1], across)

    def scale_weights(w):
        step = 128

        @pl.loop(0, depth // step)
        def _(r):
            part = pl.ds(pl.multiple_of(r * step, step), step)
            gain = jnp.broadcast_to(gain_ref[pl.ds(r, 1), :], (step, step)).T
            for n in range(w.shape[1] // step):
                lane = slice(n * step, (n + 1) * step)
                w[part, lane] = (gain * w[part, lane].astype(jnp.float32)).astype(jnp.bfloat16)

    loads[0].wait()
    loads[1].wait()
    scale_weights(wgu)
    loads[6].wait()
    columns_wait.wait_recv()
    attended_wait.wait_recv()
    summed = residual_ref[...].astype(jnp.float32)
    product = jnp.dot(attended[0], columns[:lanes, :], preferred_element_type=jnp.float32)
    for n in range(1, tp_count):
        product += jnp.dot(
            attended[n],
            columns[n * lanes : (n + 1) * lanes, :],
            preferred_element_type=jnp.float32,
        )
    stream_ref[...] = (product + summed).astype(jnp.bfloat16)
    full[:, cols] = stream_ref[...]

    stream = (full, stream_send.at[0], stream_recv.at[0])
    tp_start(*stream)

    @pl.loop(near, sp_count)
    def _(i):
        e = target(i)
        picks[e] = jnp.dot(
            chooser(e), stream_ref[...], preferred_element_type=jnp.float32
        ).astype(jnp.bfloat16)
        sp_copy(picks.at[e], arrived.at[s, :, cols], z_send.at[e], z_recv.at[s], e).start()

    loads[2].wait()
    loads[3].wait()
    scale_weights(sgu)
    tp_relay(*stream)
    tp_finish(*stream)

    @pl.loop(1, near)
    def _(i):
        e = target(i)
        picked_full[i - 1] = jnp.dot(
            chooser(e), full[...], preferred_element_type=jnp.float32
        ).astype(jnp.bfloat16)
        sp_copy(picked_full.at[i - 1], arrived.at[s], z_send.at[e], z_recv.at[s], e).start()

    arrived[s] = jnp.dot(chooser(s), full[...], preferred_element_type=jnp.float32).astype(
        jnp.bfloat16
    )

    def gated(x, w):
        wide_x = x.astype(jnp.float32)
        scale = lax.rsqrt(jnp.sum(wide_x * wide_x, axis=-1, keepdims=True) / depth + norm_eps)
        sums = jnp.dot(x, w[...], preferred_element_type=jnp.float32)
        gate = scale * sums[:, :width]
        return (gate / (1.0 + jnp.exp(-gate)) * (scale * sums[:, width:])).astype(jnp.bfloat16)

    def hidden(src):
        return hid.at[src], hid_send.at[src], hid_recv.at[src]

    def passed(src):
        return arrived.at[src], fwd_send.at[src], fwd_recv.at[src]

    shared = (shid, sh_send.at[0], sh_recv.at[0])

    def hidden_of(src):
        hid[src, :, cols] = gated(arrived[src], wgu)
        tp_start(*hidden(src))

    def pass_on(src):
        mine = arrived.at[src, :, cols]
        sp_copy(mine, mine, z_send.at[src], z_recv.at[src], src).wait_recv()
        tp_start(*passed(src))

    hidden_of(s)
    half = rows // 2

    @pl.loop(0, 2)
    def _(h):
        part = pl.ds(pl.multiple_of(h * half, half), half)
        shid[part, cols] = gated(full[part, :], sgu)

    tp_start(*shared)
    if near < sp_count:
        pass_on(source(near))
    loads[4].wait()
    loads[5].wait()

    @pl.loop(1, sp_count + LAG)
    def _(i):
        @pl.when(i + near < sp_count)
        def _():
            pass_on(source(i + near))

        @pl.when((i + near - 1 >= near) & (i + near - 1 < sp_count))
        def _():
            tp_relay(*passed(source(i + near - 1)))

        @pl.when(i < sp_count)
        def _():
            src = source(i)

            @pl.when(i < near)
            def _():
                mine = arrived.at[src]
                sp_copy(mine, mine, z_send.at[src], z_recv.at[src], src).wait_recv()

            @pl.when(i >= near)
            def _():
                tp_finish(*passed(src))

            hidden_of(src)

        @pl.when(i <= sp_count)
        def _():
            tp_relay(*hidden(source(i - 1)))

        @pl.when(i == 1)
        def _():
            tp_relay(*shared)

        @pl.when(i >= LAG)
        def _():
            src = source(i - LAG)
            tp_finish(*hidden(src))
            result = jnp.dot(hid[src], wd[...], preferred_element_type=jnp.float32).astype(
                jnp.bfloat16
            )

            @pl.when(i == LAG)
            def _():
                returned[s] = result

            @pl.when(i > LAG)
            def _():
                eout[src] = result
                sp_copy(
                    eout.at[src], returned.at[s], ret_send.at[src], ret_recv.at[s], src
                ).start()

    tp_finish(*shared)
    acc[...] = stream_ref[...].astype(jnp.float32) + jnp.dot(
        shid[...], sd[...], preferred_element_type=jnp.float32
    )

    @pl.loop(0, sp_count)
    def _(i):
        e = target(i)

        @pl.when(i > 0)
        def _():
            mine = returned.at[e]
            sp_copy(mine, mine, ret_send.at[e], ret_recv.at[e], e).wait_recv()

        picked = lax.dot_general(
            chooser(e), returned[e], (((0,), (0,)), ((), ())), preferred_element_type=jnp.float32
        )
        weight = jnp.sum(
            jnp.where(routes_row_ref[...] == e, weights_row_ref[...], 0.0), axis=0, keepdims=True
        )
        spread = jnp.broadcast_to(weight, (128, rows)).T
        for n in range(width // 128):
            lane = slice(n * 128, (n + 1) * 128)
            acc[:, lane] += spread * picked[:, lane]

    out_ref[...] = acc[...].astype(out_ref.dtype)

    tp_sent(*stream)
    columns_wait.wait_send()
    attended_wait.wait_send()

    @pl.when(s < sp_count - 1)
    def _():
        tail_copy.wait_send()

    tp_sent(*shared)

    @pl.loop(0, sp_count)
    def _(i):
        e = target(i)
        tp_sent(*hidden(e))

        @pl.when((i > 0) & (i < near))
        def _():
            mine = picked_full.at[i - 1]
            sp_copy(mine, mine, z_send.at[e], z_recv.at[e], e).wait_send()

        @pl.when(i >= near)
        def _():
            sp_copy(picks.at[e], picks.at[e], z_send.at[e], z_recv.at[e], e).wait_send()

            tp_sent(*passed(source(i)))

        @pl.when(i > 0)
        def _():
            sp_copy(eout.at[e], eout.at[e], ret_send.at[e], ret_recv.at[e], e).wait_send()


def per_device(
    queries,
    keys_values,
    sink_logits,
    proj_weight,
    residual,
    norm_gain,
    routes,
    route_weights,
    gate_weight,
    up_weight,
    down_weight,
    shared_gate,
    shared_up,
    shared_down,
):
    sp_count = lax.axis_size("sp")
    tp_count = lax.axis_size("tp")
    rows, width = residual.shape
    depth = width * tp_count
    cap = 2 * rows * TOP_K // sp_count
    kv_width = keys_values.shape[2]
    bf16 = jnp.bfloat16
    vmem = pl.BlockSpec(memory_space=pltpu.VMEM)
    hbm = pl.BlockSpec(memory_space=pl.ANY)
    dma = pltpu.SemaphoreType.DMA
    return pl.pallas_call(
        functools.partial(expert_kernel, sp_count, tp_count, cap),
        out_shape=jax.ShapeDtypeStruct((rows, width), bf16),
        in_specs=[vmem] * 7 + [hbm] * 7,
        out_specs=vmem,
        scratch_shapes=[
            pltpu.VMEM((depth, 2 * width), bf16),
            pltpu.VMEM((depth, width), bf16),
            pltpu.VMEM((depth, 2 * width), bf16),
            pltpu.VMEM((depth, width), bf16),
            pltpu.VMEM((rows, depth), bf16),
            pltpu.VMEM((sp_count, cap, width), bf16),
            pltpu.VMEM((max(1, min(NEAR, sp_count) - 1), cap, depth), bf16),
            pltpu.VMEM((sp_count, cap, depth), bf16),
            pltpu.VMEM((sp_count, cap, depth), bf16),
            pltpu.VMEM((rows, depth), bf16),
            pltpu.VMEM((sp_count, cap, width), bf16),
            pltpu.VMEM((sp_count, cap, width), bf16),
            pltpu.VMEM((sp_count, rows), jnp.int32),
            pltpu.VMEM((rows, width), jnp.float32),
            pltpu.VMEM((rows, width), bf16),
            pltpu.VMEM((2, WINDOW, kv_width), bf16),
            pltpu.VMEM((2, WINDOW + rows, HEAD_WIDTH), bf16),
            pltpu.VMEM((tp_count,) + queries.shape, bf16),
            pltpu.VMEM((tp_count * proj_weight.shape[0], width), bf16),
            dma((7,)),
            dma((3,)),
            dma((3,)),
            dma((1,)),
            dma((1, 3)),
            dma((sp_count,)),
            dma((sp_count,)),
            dma((sp_count,)),
            dma((sp_count, 3)),
            dma((sp_count,)),
            dma((sp_count, 3)),
            dma((1,)),
            dma((1, 3)),
            dma((sp_count,)),
            dma((sp_count,)),
        ],
        compiler_params=pltpu.CompilerParams(
            collective_id=0, has_side_effects=True, vmem_limit_bytes=56 * 1024 * 1024
        ),
    )(
        queries,
        keys_values,
        sink_logits[None, :],
        residual,
        routes.T,
        route_weights.T,
        norm_gain.reshape(-1, 128),
        proj_weight,
        gate_weight,
        up_weight,
        down_weight,
        shared_gate,
        shared_up,
        shared_down,
    )


def solution(mesh):
    placed = (
        P("sp", "tp"),
        P(None, "sp", None),
        P("tp"),
        P("tp", None),
        P("sp", "tp"),
        P(),
        P("sp", None),
        P("sp", None),
        P("sp", None, "tp"),
        P("sp", None, "tp"),
        P("sp", None, "tp"),
        P(None, "tp"),
        P(None, "tp"),
        P(None, "tp"),
    )
    return jax.shard_map(
        per_device, mesh=mesh, in_specs=placed, out_specs=P("sp", "tp"), check_vma=False
    )
```
